32 devices in a mesh: grp: 2 (over y), ep: 4 (over z), tp: 4 (over x, core).
Axes of the slice: x: 2, y: 2, z: 4, core: 2. Of those that a mesh axis runs over, the one named last changes fastest.
Arguments:
- tokens: bfloat16 [4096, 2048], P(('grp', 'ep', 'tp')), parts along dimension 0, may hold values from -6 to 6
- norm_gain: float32 [2048], replicated, may hold values from 0.1 to 1.9
- route_ids: int32 [4096, 2], P(('grp', 'ep', 'tp')), parts along dimension 0, may hold values from 0 to 15, all different within a row; in each aligned block of 128 rows (0 to 127, 128 to 255, ...) at most 24 rows name the same one
- route_weights: float32 [4096, 2], P(('grp', 'ep', 'tp')), parts along dimension 0, may hold values from 0.1 to 0.9
- w_gate: bfloat16 [16, 2048, 512], P(('ep', 'tp')), may hold values from -0.125 to 0.125
- w_up: bfloat16 [16, 2048, 512], P(('ep', 'tp')), may hold values from -0.125 to 0.125
- w_down: bfloat16 [16, 512, 2048], P(('ep', 'tp')), may hold values from -0.25 to 0.25
Outputs:
- mixed: bfloat16 [4096, 2048], P(('grp', 'ep', 'tp')), parts along dimension 0
The draws below stay inside these ranges and needn't reach their ends.
There are 2 independent parts, one for each index of `grp`. The reference program is written for one: setup_inputs(seed, part) draws one part's arguments, and reference() takes and returns one part's arrays. A program takes and returns all parts, laid end to end along the dimension named above; an argument that names none is the same for every part. Nothing has to cross between parts.
Inputs may be any that keep to these rules, and one draw needn't show every extreme that they name: `route_ids`: each token names 2 different experts. Among the tokens of one device (aligned blocks of 128 tokens) no expert is named more than 24 times, a bound that some block reaches.
All inputs are finite; a program needn't handle non-finite values.
Results may differ from the reference program's by a relative error of at most 0.0071.
Values may be sent and summed in bfloat16 or wider, within the bound.
A program may use at most 64 MiB of HBM per device.

```python
import math
import jax
import jax.numpy as jnp
import numpy as np
from jax import lax

D = 2048
FF = 512
TOP = 2
TOK_DEV = 128
EXPERTS = 16
CAP = 24
TOKENS = 2048


def block_scale(own_key, shape, shards, least, high):
    loudness, own = 1.0, jax.random.fold_in(own_key, 6)
    for dim, shards_of in shards:
        heights = jnp.exp(jax.random.uniform(jax.random.fold_in(own, dim), (shards_of,), jnp.float32, least / len(shards), high / len(shards)))
        loudness = loudness * jnp.repeat(heights, shape[dim] // shards_of).reshape([-1 if axis == dim else 1 for axis in range(len(shape))])
    return loudness


def routed_block(key, own, number, rows, amount, top, limit, skew):
    order = jax.random.permutation(key, amount)
    packed, ordinary = load_shares(amount, rows * top, limit, skew, True), load_shares(amount, rows * top, limit, skew, False)
    places = jnp.arange(amount)

    def named(lengths, turn):
        used = int((lengths > 0).sum())
        fixed = max(1, used // 4)
        shifted = fixed + (places - fixed + turn * (used - fixed)) % max(1, amount - fixed)
        return jnp.zeros((amount,), jnp.int32).at[order[jnp.where(places < fixed, places, shifted)]].set(jnp.asarray(lengths, jnp.int32))

    lengths = jnp.where(number % 4 == 0, named(packed, number // 4), named(ordinary, number - number // 4 - 1))
    mixed = jax.random.permutation(jax.random.fold_in(own, 3), amount)
    source_of, sink = mixed[0:amount // 2 * 2:2], mixed[1:amount // 2 * 2:2]
    slack = jnp.minimum(lengths[source_of] - 1, limit - lengths[sink]) // 2
    slack = jnp.where((source_of == order[0]) | (sink == order[0]) | (lengths[sink] == 0), 0, jnp.maximum(slack, 0))
    shifted = jax.random.randint(jax.random.fold_in(own, 4), (amount // 2,), 0, 1 << 20) % (slack + 1)
    lengths = lengths.at[source_of].add(-shifted).at[sink].add(shifted)
    labels = jnp.searchsorted(jnp.cumsum(lengths), jnp.arange(rows * top), side="right").astype(jnp.int32)
    table = labels.reshape(top, rows).T
    table = table[jax.random.permutation(jax.random.fold_in(own, 1), rows)]
    turn = jax.random.randint(jax.random.fold_in(own, 2), (rows, 1), 0, top)
    return jnp.take_along_axis(table, (jnp.arange(top)[None, :] + turn) % top, axis=1)


def load_shares(number_of, total, most, lean, full):
    portions = [(1 << 20) // math.isqrt(rank ** lean) + 1 for rank in range(1, number_of + 1)]
    largest = most if full else min(most, max(-(-total // number_of), total * portions[0] // sum(portions)))
    least = 1 if total - largest >= number_of - 1 else 0
    holding, surplus = [largest] + [least] * (number_of - 1), total - largest - least * (number_of - 1)
    while surplus > 0:
        movable = [i for i in range(1, number_of) if holding[i] < largest] or [i for i in range(1, number_of) if holding[i] < most]
        pool, left = sum([portions[i] for i in movable]), surplus
        for i in movable:
            more = min(most - holding[i], max(1, left * portions[i] // pool), surplus)
            holding[i] = holding[i] + more
            surplus = surplus - more
    return np.array(holding)


def centred(stream_key, extent, deviation, most, pieces=(), kind=jnp.bfloat16):
    loudness = block_scale(stream_key, extent, pieces, -0.22, 0.18) if pieces else 1.0
    values = jax.random.normal(stream_key, extent, jnp.float32) * deviation * loudness
    return jnp.minimum(jnp.maximum(values, -most), most).astype(kind)


def setup_inputs(seed: int = 0, part: int = 0) -> dict:
    key_list = jax.random.split(jax.random.key(seed), 8)
    own_keys = jax.random.split(jax.random.fold_in(key_list[7], part), 8)
    tokens = centred(own_keys[0], (TOKENS, D), 1.0, 6.0, ((0, 16),))
    norm_gain = jnp.clip(1.0 + 0.18 * jax.random.normal(key_list[1], (D,), jnp.float32), 0.1, 1.9)
    route_ids_keys = jax.random.split(jax.random.fold_in(own_keys[2], 1), TOKENS // TOK_DEV)
    route_ids_turns = jax.random.permutation(jax.random.fold_in(own_keys[2], 3), TOKENS // TOK_DEV)
    route_ids = jax.vmap(lambda own, number: routed_block(jax.random.fold_in(own_keys[2], 2), own, number, TOK_DEV, EXPERTS, TOP, CAP, 2))(route_ids_keys, route_ids_turns).reshape((TOKENS, TOP))
    route_weights = jnp.clip(0.1 + 0.79999997 * jax.random.uniform(own_keys[3], (TOKENS, TOP), jnp.float32) ** block_scale(own_keys[3], (TOKENS, TOP), ((0, 16),), -0.2, 0.2), 0.1, 0.9)
    w_gate = centred(key_list[4], (EXPERTS, D, FF), D ** -0.5, 0.125, ((0, 16),))
    w_up = centred(key_list[5], (EXPERTS, D, FF), D ** -0.5, 0.125, ((0, 16),))
    w_down = centred(key_list[6], (EXPERTS, FF, D), FF ** -0.5, 0.25, ((0, 16),))
    return {"tokens": tokens, "norm_gain": norm_gain, "route_ids": route_ids, "route_weights": route_weights, "w_gate": w_gate, "w_up": w_up, "w_down": w_down}


def reference(tokens, norm_gain, route_ids, route_weights, w_gate, w_up, w_down):
    source_count = TOKENS // TOK_DEV
    values = tokens.astype(jnp.float32)
    normed = (values * lax.rsqrt(lax.optimization_barrier(jnp.mean(values * values, axis=-1, keepdims=True)) + 1e-06) * norm_gain).astype(jnp.bfloat16)
    per_device = route_ids.reshape(source_count, TOK_DEV * TOP)
    onehot = (per_device[:, :, None] == jnp.arange(EXPERTS, dtype=jnp.int32)[None, None, :]).astype(jnp.int32)
    slot_index = lax.optimization_barrier(jnp.sum((jnp.cumsum(onehot, axis=1) - onehot) * onehot, axis=-1))
    position = (jnp.arange(source_count, dtype=jnp.int32)[:, None] * CAP + slot_index).reshape(-1).astype(jnp.int32)
    flat_ids = route_ids.reshape(-1)
    total_rows = TOKENS * TOP
    row_table = jnp.full((EXPERTS, source_count * CAP), total_rows, jnp.int32)
    row_table = row_table.at[flat_ids, position].set(jnp.arange(total_rows, dtype=jnp.int32))

    def apply_expert(carry, operand):
        table_row, gate_w, up_w, down_w = operand
        token_rows = normed[jnp.minimum(table_row // TOP, TOKENS - 1)]
        gate_act = jnp.dot(token_rows, gate_w, preferred_element_type=jnp.float32)
        up_act = jnp.dot(token_rows, up_w, preferred_element_type=jnp.float32)
        hidden = (jax.nn.silu(gate_act) * up_act).astype(jnp.bfloat16)
        result = jnp.dot(hidden, down_w, preferred_element_type=jnp.float32).astype(jnp.bfloat16)
        return (carry.at[table_row].set(result), None)
    start = jnp.zeros((total_rows + 1, D), jnp.bfloat16)
    picked, _ = lax.scan(apply_expert, start, (row_table, w_gate, w_up, w_down))
    picked = picked[:total_rows].reshape(TOKENS, TOP, D).astype(jnp.float32)
    return lax.optimization_barrier(jnp.sum(picked * route_weights[:, :, None], axis=1)).astype(jnp.bfloat16)
```

```python
import functools

import jax
import jax.numpy as jnp
from jax import lax
from jax.experimental import pallas as pl
from jax.experimental.pallas import tpu as pltpu
from jax.sharding import PartitionSpec as P

MESH = pl.DeviceIdType.MESH


def plain(tokens, norm_gain, route_ids, route_weights, w_gate, w_up, w_down):
    tok_rows, model_width = tokens.shape
    top_count = route_ids.shape[1]
    ep_count = lax.axis_size("ep")
    tp_count = lax.axis_size("tp")
    experts = ep_count * tp_count
    capacity = 3 * tok_rows * top_count // (2 * experts)
    values = tokens.astype(jnp.float32)
    normed = (
        values * lax.rsqrt(jnp.mean(values * values, axis=-1, keepdims=True) + 1e-06) * norm_gain
    ).astype(jnp.bfloat16)
    flat_ids = route_ids.reshape(-1)
    onehot = (flat_ids[:, None] == jnp.arange(experts, dtype=jnp.int32)[None, :]).astype(jnp.int32)
    slot_index = jnp.sum((jnp.cumsum(onehot, axis=0) - onehot) * onehot, axis=-1)
    token_of = jnp.arange(tok_rows * top_count, dtype=jnp.int32) // top_count
    buffer = jnp.zeros((experts, capacity, model_width), jnp.bfloat16)
    buffer = buffer.at[flat_ids, slot_index].set(normed[token_of])
    received = lax.all_to_all(buffer, ("ep", "tp"), split_axis=0, concat_axis=0, tiled=True)
    flat_rows = received.reshape(-1, model_width)
    gate_act = jnp.dot(flat_rows, w_gate[0], preferred_element_type=jnp.float32)
    up_act = jnp.dot(flat_rows, w_up[0], preferred_element_type=jnp.float32)
    hidden = (jax.nn.silu(gate_act) * up_act).astype(jnp.bfloat16)
    result = jnp.dot(hidden, w_down[0], preferred_element_type=jnp.float32).astype(jnp.bfloat16)
    returned = lax.all_to_all(
        result.reshape(received.shape), ("ep", "tp"), split_axis=0, concat_axis=0, tiled=True
    )
    picked = (
        returned[flat_ids, slot_index].reshape(tok_rows, top_count, model_width).astype(jnp.float32)
    )
    return jnp.sum(picked * route_weights[:, :, None], axis=1).astype(jnp.bfloat16)


def flipped(index, bits):
    bit = 1
    while bit <= bits:
        if bits & bit:
            index = index + (1 - 2 * ((index // bit) % 2)) * bit
        bit *= 2
    return index


def kernel(
    ep_count, tp_count, cap,
    x_ref, gain_ref, ids_ref, wts_ref, wg_hbm, wu_hbm, wd_hbm, out_ref,
    send, recv, res, back, wg, wu, wd, comb_hi, comb_lo, acc,
    w_sem, send_sem, recv_sem, ret_sem, back_sem,
):
    ep, tp, grp = lax.axis_index("ep"), lax.axis_index("tp"), lax.axis_index("grp")
    rows, width = x_ref.shape
    top = ids_ref.shape[1]
    experts = ep_count * tp_count
    me = ep * tp_count + tp

    def peer(g):
        return (grp, flipped(ep, g // tp_count), flipped(tp, g % tp_count))

    barrier = pltpu.get_barrier_semaphore()
    for g in range(1, experts):
        pl.semaphore_signal(barrier, inc=1, device_id=peer(g), device_id_type=MESH)
    loads = [
        pltpu.make_async_copy(src.at[0], dst, w_sem.at[i])
        for i, (src, dst) in enumerate(((wg_hbm, wg), (wu_hbm, wu), (wd_hbm, wd)))
    ]
    for load in loads:
        load.start()

    down = lax.broadcasted_iota(jnp.int32, (rows, rows), 0)
    across = lax.broadcasted_iota(jnp.int32, (rows, rows), 1)

    def as_row(column):
        return jnp.sum(jnp.where(down == across, column, 0), axis=0, keepdims=True)

    expert_of = lax.broadcasted_iota(jnp.int32, (experts, rows), 0) ^ me
    ids, wts = ids_ref[...], wts_ref[...]
    named = jnp.zeros((experts, rows), jnp.float32)
    weight = jnp.zeros((experts, rows), jnp.float32)
    for k in range(top):
        match = as_row(ids[:, k:k + 1]) == expert_of
        named = named + jnp.where(match, 1.0, 0.0)
        weight = weight + jnp.where(match, as_row(wts[:, k:k + 1]), 0.0)
    earlier = jnp.where(down < across, 1.0, 0.0).astype(jnp.bfloat16)
    rank = jnp.dot(named.astype(jnp.bfloat16), earlier, preferred_element_type=jnp.float32)
    rank = jnp.where(named > 0.5, rank, -1.0)
    slot = lax.broadcasted_iota(jnp.int32, (experts, cap, rows), 1).astype(jnp.float32)
    taken = rank[:, None, :] == slot
    pick = jnp.where(taken, 1.0, 0.0).reshape(experts * cap, rows).astype(jnp.bfloat16)
    share = jnp.where(taken, weight[:, None, :], 0.0).reshape(experts * cap, rows)
    share_hi = share.astype(jnp.bfloat16)
    comb_hi[...] = share_hi
    comb_lo[...] = (share - share_hi.astype(jnp.float32)).astype(jnp.bfloat16)

    values = x_ref[...].astype(jnp.float32)
    normed = (
        values
        * lax.rsqrt(jnp.mean(values * values, axis=-1, keepdims=True) + 1e-06)
        * gain_ref[...]
    ).astype(jnp.bfloat16)

    pl.semaphore_wait(barrier, experts - 1)
    out_copies, ret_copies = {}, {}

    def start_group(r):
        for g in range(r * tp_count, (r + 1) * tp_count):
            if g:
                out_copies[g].start()

    order = list(range(ep_count - 1, -1, -1))
    for r in order:
        base = r * tp_count
        packed = jnp.dot(
            pick[base * cap:(base + tp_count) * cap], normed, preferred_element_type=jnp.float32
        ).astype(jnp.bfloat16).reshape(tp_count, cap, width)
        for j in range(tp_count):
            g = base + j
            if g == 0:
                recv[0] = packed[0]
            else:
                send[g] = packed[j]
                out_copies[g] = pltpu.make_async_remote_copy(
                    src_ref=send.at[g], dst_ref=recv.at[g],
                    send_sem=send_sem.at[g], recv_sem=recv_sem.at[g],
                    device_id=peer(g), device_id_type=MESH,
                )
        start_group(r)
    for load in loads:
        load.wait()

    for r in order:
        base = r * tp_count
        for g in range(base, base + tp_count):
            if g:
                out_copies[g].wait_recv()
        block = recv[base:base + tp_count].reshape(tp_count * cap, width)
        gate_act = jnp.dot(block, wg[...], preferred_element_type=jnp.float32)
        up_act = jnp.dot(block, wu[...], preferred_element_type=jnp.float32)
        hidden = (gate_act / (1.0 + jnp.exp(-gate_act)) * up_act).astype(jnp.bfloat16)
        result = jnp.dot(hidden, wd[...], preferred_element_type=jnp.float32)
        result = result.astype(jnp.bfloat16).reshape(tp_count, cap, width)
        for j in range(tp_count):
            g = base + j
            if g == 0:
                back[0] = result[0]
            else:
                res[g] = result[j]
                ret_copies[g] = pltpu.make_async_remote_copy(
                    src_ref=res.at[g], dst_ref=back.at[g],
                    send_sem=ret_sem.at[g], recv_sem=back_sem.at[g],
                    device_id=peer(g), device_id_type=MESH,
                )
                ret_copies[g].start()

    for step, r in enumerate(order):
        base = r * tp_count
        for g in range(base, base + tp_count):
            if g:
                ret_copies[g].wait_recv()
        block = back[base:base + tp_count].reshape(tp_count * cap, width)
        part = sum(
            lax.dot_general(
                comb[base * cap:(base + tp_count) * cap, :], block,
                (((0,), (0,)), ((), ())), preferred_element_type=jnp.float32,
            )
            for comb in (comb_hi, comb_lo)
        )
        if step == 0:
            acc[...] = part
        elif step < ep_count - 1:
            acc[...] += part
        else:
            out_ref[...] = (acc[...] + part).astype(out_ref.dtype)
    for g in range(1, experts):
        out_copies[g].wait_send()
        ret_copies[g].wait_send()


def fused(ep_count, tp_count, tokens, norm_gain, route_ids, route_weights, w_gate, w_up, w_down):
    rows, width = tokens.shape
    hidden = w_gate.shape[2]
    experts = ep_count * tp_count
    cap = 3 * rows * route_ids.shape[1] // (2 * experts)
    vmem = pl.BlockSpec(memory_space=pltpu.VMEM)
    hbm = pl.BlockSpec(memory_space=pl.ANY)
    slots = pltpu.VMEM((experts, cap, width), jnp.bfloat16)
    sems = pltpu.SemaphoreType.DMA((experts,))
    return pl.pallas_call(
        functools.partial(kernel, ep_count, tp_count, cap),
        out_shape=jax.ShapeDtypeStruct((rows, width), tokens.dtype),
        in_specs=[vmem] * 4 + [hbm] * 3,
        out_specs=vmem,
        scratch_shapes=[
            slots, slots, slots, slots,
            pltpu.VMEM((width, hidden), jnp.bfloat16),
            pltpu.VMEM((width, hidden), jnp.bfloat16),
            pltpu.VMEM((hidden, width), jnp.bfloat16),
            pltpu.VMEM((experts * cap, rows), jnp.bfloat16),
            pltpu.VMEM((experts * cap, rows), jnp.bfloat16),
            pltpu.VMEM((rows, width), jnp.float32),
            pltpu.SemaphoreType.DMA((3,)),
            sems, sems, sems, sems,
        ],
        compiler_params=pltpu.CompilerParams(
            collective_id=0, has_side_effects=True, vmem_limit_bytes=56 * 1024 * 1024
        ),
    )(tokens, norm_gain.reshape(1, width), route_ids, route_weights, w_gate, w_up, w_down)


def solution(mesh):
    ep_count, tp_count = mesh.shape["ep"], mesh.shape["tp"]

    def on_device(*args):
        rows, experts = args[0].shape[0], ep_count * tp_count
        cap = 3 * rows * args[2].shape[1] // (2 * experts)
        if cap % 8 or rows % 128 or experts & (experts - 1) or experts > 32:
            return plain(*args)
        return fused(ep_count, tp_count, *args)

    return jax.shard_map(
        on_device,
        mesh=mesh,
        in_specs=(
            P(("grp", "ep", "tp"), None),
            P(),
            P(("grp", "ep", "tp"), None),
            P(("grp", "ep", "tp"), None),
            P(("ep", "tp"), None, None),
            P(("ep", "tp"), None, None),
            P(("ep", "tp"), None, None),
        ),
        out_specs=P(("grp", "ep", "tp"), None),
        check_vma=False,
    )
```

```python
import functools

import jax
import jax.numpy as jnp
from jax import lax
from jax.experimental import pallas as pl
from jax.experimental.pallas import tpu as pltpu
from jax.sharding import PartitionSpec as P

MESH = pl.DeviceIdType.MESH


def plain(tokens, norm_gain, route_ids, route_weights, w_gate, w_up, w_down):
    tok_rows, model_width = tokens.shape
    top_count = route_ids.shape[1]
    ep_count = lax.axis_size("ep")
    tp_count = lax.axis_size("tp")
    experts = ep_count * tp_count
    capacity = 3 * tok_rows * top_count // (2 * experts)
    values = tokens.astype(jnp.float32)
    normed = (
        values * lax.rsqrt(jnp.mean(values * values, axis=-1, keepdims=True) + 1e-06) * norm_gain
    ).astype(jnp.bfloat16)
    flat_ids = route_ids.reshape(-1)
    onehot = (flat_ids[:, None] == jnp.arange(experts, dtype=jnp.int32)[None, :]).astype(jnp.int32)
    slot_index = jnp.sum((jnp.cumsum(onehot, axis=0) - onehot) * onehot, axis=-1)
    token_of = jnp.arange(tok_rows * top_count, dtype=jnp.int32) // top_count
    buffer = jnp.zeros((experts, capacity, model_width), jnp.bfloat16)
    buffer = buffer.at[flat_ids, slot_index].set(normed[token_of])
    received = lax.all_to_all(buffer, ("ep", "tp"), split_axis=0, concat_axis=0, tiled=True)
    flat_rows = received.reshape(-1, model_width)
    gate_act = jnp.dot(flat_rows, w_gate[0], preferred_element_type=jnp.float32)
    up_act = jnp.dot(flat_rows, w_up[0], preferred_element_type=jnp.float32)
    hidden = (jax.nn.silu(gate_act) * up_act).astype(jnp.bfloat16)
    result = jnp.dot(hidden, w_down[0], preferred_element_type=jnp.float32).astype(jnp.bfloat16)
    returned = lax.all_to_all(
        result.reshape(received.shape), ("ep", "tp"), split_axis=0, concat_axis=0, tiled=True
    )
    picked = (
        returned[flat_ids, slot_index].reshape(tok_rows, top_count, model_width).astype(jnp.float32)
    )
    return jnp.sum(picked * route_weights[:, :, None], axis=1).astype(jnp.bfloat16)


def flipped(index, bits):
    bit = 1
    while bit <= bits:
        if bits & bit:
            index = index + (1 - 2 * ((index // bit) % 2)) * bit
        bit *= 2
    return index


PIECES = 2


def kernel(
    ep_count, tp_count, cap,
    x_ref, gain_ref, ids_ref, wts_ref, wg_hbm, wu_hbm, wd_hbm, out_ref,
    normed, meta, share_hi, share_lo, nsend, nrecv, nres, nback,
    rblock, rmeta, rpick, rshare_hi, rshare_lo, fsend, frecv, fres, rback, rsend, farback,
    wg, wu, wd, acc,
    w_sem, dense_s, dense_r, meta_s, meta_r, near_s, near_r, nret_s, nret_r,
    far_s, far_r, fret_s, fret_r, final_s, final_r,
):
    ep, tp, grp = lax.axis_index("ep"), lax.axis_index("tp"), lax.axis_index("grp")
    rows, width = x_ref.shape
    part_w = width // PIECES
    top = ids_ref.shape[1]
    experts = ep_count * tp_count
    near = 2 * tp_count
    me = ep * tp_count + tp
    boundary = (ep + ep // 2) % 2
    wave_of_me = 1 - boundary
    own_relay, other_relay = 1 + ep // 2, 2 - ep // 2
    is_boundary, is_end = boundary == 1, boundary == 0

    def at(plane, j):
        return (grp, plane, flipped(tp, j))

    def remote(src, dst, s_sem, r_sem, target):
        return pltpu.make_async_remote_copy(
            src_ref=src, dst_ref=dst, send_sem=s_sem, recv_sem=r_sem,
            device_id=target, device_id_type=MESH,
        )

    barrier = pltpu.get_barrier_semaphore()
    for g in range(1, experts):
        pl.semaphore_signal(
            barrier, inc=1, device_id=at(flipped(ep, g // tp_count), g % tp_count),
            device_id_type=MESH,
        )
    loads = [
        pltpu.make_async_copy(src.at[0], dst, w_sem.at[i])
        for i, (src, dst) in enumerate(((wg_hbm, wg), (wu_hbm, wu), (wd_hbm, wd)))
    ]
    for load in loads:
        load.start()

    planes = [ep, flipped(ep, 1)]
    dense = [
        remote(normed.at[c], rblock.at[wave_of_me, c], dense_s.at[c], dense_r.at[wave_of_me, c],
               at(other_relay, 0))
        for c in range(PIECES)
    ]
    meta_copy = remote(meta, rmeta.at[wave_of_me], meta_s.at[0], meta_r.at[wave_of_me],
                       at(other_relay, 0))
    near_out = [
        remote(nsend.at[g], nrecv.at[g], near_s.at[g], near_r.at[g],
               at(planes[g // tp_count], g % tp_count))
        for g in range(near)
    ]
    near_ret = [
        remote(nres.at[g], nback.at[g], nret_s.at[g], nret_r.at[g],
               at(planes[g // tp_count], g % tp_count))
        for g in range(near)
    ]
    far_out, far_ret, final = {}, {}, {}
    for v in range(2):
        for c in range(PIECES):
            for i in range(near):
                far_out[v, c, i] = remote(
                    fsend.at[v, c, i], frecv.at[v, c, i % tp_count], far_s.at[v, c, i],
                    far_r.at[v, c, i % tp_count], at(planes[i // tp_count], i % tp_count))
            for j in range(tp_count):
                place = wave_of_me * tp_count + j
                far_ret[v, c, j] = remote(
                    fres.at[v, c, j], rback.at[v, c, place], fret_s.at[v, c, j],
                    fret_r.at[v, c, place], at(own_relay, j))
            final[v, c] = remote(rsend.at[v, c], farback.at[c], final_s.at[v, c], final_r.at[c],
                                 at(flipped(ep, 3 - v), 0))

    values = x_ref[...].astype(jnp.float32)
    rows_normed = (
        values
        * lax.rsqrt(jnp.mean(values * values, axis=-1, keepdims=True) + 1e-06)
        * gain_ref[...]
    ).astype(jnp.bfloat16)
    for c in range(PIECES):
        normed[c] = rows_normed[:, c * part_w:(c + 1) * part_w]

    down = lax.broadcasted_iota(jnp.int32, (rows, rows), 0)
    across = lax.broadcasted_iota(jnp.int32, (rows, rows), 1)

    def as_row(column):
        return jnp.sum(jnp.where(down == across, column, 0), axis=0, keepdims=True)

    expert_of = lax.broadcasted_iota(jnp.int32, (experts, rows), 0) ^ me
    ids, wts = ids_ref[...], wts_ref[...]
    named = jnp.zeros((experts, rows), jnp.float32)
    weight = jnp.zeros((experts, rows), jnp.float32)
    for k in range(top):
        match = as_row(ids[:, k:k + 1]) == expert_of
        named = named + jnp.where(match, 1.0, 0.0)
        weight = weight + jnp.where(match, as_row(wts[:, k:k + 1]), 0.0)
    earlier = jnp.where(down < across, 1.0, 0.0).astype(jnp.bfloat16)
    rank = jnp.dot(named.astype(jnp.bfloat16), earlier, preferred_element_type=jnp.float32)
    rank = jnp.where(named > 0.5, rank, -1.0)
    meta[0:near] = rank[near:]
    meta[near:] = weight[near:]

    def onehots(rank, weight):
        slot = lax.broadcasted_iota(jnp.int32, (near, cap, rows), 1).astype(jnp.float32)
        taken = rank[:, None, :] == slot
        pick = jnp.where(taken, 1.0, 0.0).reshape(near * cap, rows).astype(jnp.bfloat16)
        share = jnp.where(taken, weight[:, None, :], 0.0).reshape(near * cap, rows)
        high = share.astype(jnp.bfloat16)
        return pick, high, (share - high.astype(jnp.float32)).astype(jnp.bfloat16)

    pl.semaphore_wait(barrier, experts - 1)

    @pl.when(is_boundary)
    def _():
        meta_copy.start()
        for c in range(PIECES):
            dense[c].start()

    pick, high, low = onehots(rank[:near], weight[:near])
    share_hi[...] = high
    share_lo[...] = low

    def pack_near(p):
        packed = jnp.dot(
            pick[p * tp_count * cap:(p + 1) * tp_count * cap], rows_normed,
            preferred_element_type=jnp.float32,
        ).astype(jnp.bfloat16).reshape(tp_count, cap, width)
        for j in range(tp_count):
            g = p * tp_count + j
            if g:
                nsend[g] = packed[j]
            else:
                nrecv[0] = packed[0]
        for j in range(tp_count):
            if p or j:
                near_out[p * tp_count + j].start()

    pack_near(1)

    @pl.when(is_end)
    def _():
        meta_copy.start()
        for c in range(PIECES):
            dense[c].start()

    pack_near(0)

    def hidden_of(gate_act, up_act):
        return (gate_act / (1.0 + jnp.exp(-gate_act)) * up_act).astype(jnp.bfloat16)

    def dot(a, b):
        return jnp.dot(a, b, preferred_element_type=jnp.float32)

    def expert_near(p):
        base = p * tp_count
        for g in range(base, base + tp_count):
            if g:
                near_out[g].wait_recv()
        block = nrecv[base:base + tp_count].reshape(tp_count * cap, width)
        hidden = hidden_of(dot(block, wg[...]), dot(block, wu[...]))
        result = dot(hidden, wd[...]).astype(jnp.bfloat16).reshape(tp_count, cap, width)
        for j in range(tp_count):
            if p or j:
                nres[base + j] = result[j]
            else:
                nback[0] = result[0]
        for j in range(tp_count):
            if p or j:
                near_ret[base + j].start()

    def relay_out(v, c):
        @pl.when(is_boundary)
        def _():
            if c == 0:
                remote(meta, rmeta.at[v], meta_s.at[0], meta_r.at[v], at(other_relay, 0)).wait_recv()
                ranks, weights = rmeta[v, 0:near], rmeta[v, near:]
                if v == 0:
                    ranks = jnp.concatenate([ranks[tp_count:], ranks[:tp_count]], axis=0)
                    weights = jnp.concatenate([weights[tp_count:], weights[:tp_count]], axis=0)
                rp, rh, rl = onehots(ranks, weights)
                rpick[v] = rp
                rshare_hi[v] = rh
                rshare_lo[v] = rl
            remote(normed.at[c], rblock.at[v, c], dense_s.at[c], dense_r.at[v, c],
                   at(other_relay, 0)).wait_recv()
            packed = dot(rpick[v], rblock[v, c]).astype(jnp.bfloat16).reshape(near, cap, part_w)
            frecv[v, c, 0] = packed[0]
            for i in range(1, near):
                fsend[v, c, i] = packed[i]
            for i in list(range(tp_count, near)) + list(range(1, tp_count)):
                far_out[v, c, i].start()

    def expert_far(v):
        gate_act = up_act = None
        for c in range(PIECES):
            for j in range(1, tp_count):
                far_out[v, c, j].wait_recv()

            @pl.when(is_end)
            def _():
                far_out[v, c, tp_count].wait_recv()

            block = frecv[v, c].reshape(tp_count * cap, part_w)
            more_gate = dot(block, wg[c * part_w:(c + 1) * part_w])
            more_up = dot(block, wu[c * part_w:(c + 1) * part_w])
            gate_act = more_gate if c == 0 else gate_act + more_gate
            up_act = more_up if c == 0 else up_act + more_up
        hidden = hidden_of(gate_act, up_act)
        for c in range(PIECES):
            result = dot(hidden, wd[:, c * part_w:(c + 1) * part_w])
            result = result.astype(jnp.bfloat16).reshape(tp_count, cap, part_w)
            fres[v, c] = result
            for j in range(1, tp_count):
                far_ret[v, c, j].start()

            @pl.when(is_end)
            def _():
                far_ret[v, c, 0].start()

            @pl.when(is_boundary)
            def _():
                rback[v, c, 0] = fres[v, c, 0]

    def combine(high, low, block):
        total = None
        for comb in (high, low):
            term = lax.dot_general(
                comb, block, (((0,), (0,)), ((), ())), preferred_element_type=jnp.float32
            )
            total = term if total is None else total + term
        return total

    def relay_back(v, c):
        @pl.when(is_boundary)
        def _():
            for i in range(1, near):
                remote(fres.at[v, c, 0], rback.at[v, c, i], fret_s.at[v, c, 0],
                       fret_r.at[v, c, i], at(own_relay, 1)).wait_recv()
            block = rback[v, c].reshape(near * cap, part_w)
            rsend[v, c] = combine(rshare_hi[v], rshare_lo[v], block).astype(jnp.bfloat16)
            final[v, c].start()

    for load in loads:
        load.wait()
    expert_near(0)
    relay_out(0, 0)
    expert_near(1)
    for c in range(1, PIECES):
        relay_out(0, c)
    relay_out(1, 0)
    expert_far(0)
    for c in range(1, PIECES):
        relay_out(1, c)
    relay_back(0, 0)
    expert_far(1)
    for c in range(1, PIECES):
        relay_back(0, c)

    for g in range(1, near):
        near_ret[g].wait_recv()
    acc[...] = combine(share_hi[...], share_lo[...], nback[...].reshape(near * cap, width))
    for c in range(PIECES):
        relay_back(1, c)
    for c in range(PIECES):
        final[0, c].wait_recv()
        part = acc[:, c * part_w:(c + 1) * part_w] + farback[c].astype(jnp.float32)
        out_ref[:, c * part_w:(c + 1) * part_w] = part.astype(out_ref.dtype)

    meta_copy.wait_send()
    for copy in dense + near_out[1:] + near_ret[1:]:
        copy.wait_send()
    for v in range(2):
        for c in range(PIECES):
            for j in range(1, tp_count):
                far_ret[v, c, j].wait_send()

    @pl.when(is_end)
    def _():
        for v in range(2):
            for c in range(PIECES):
                far_ret[v, c, 0].wait_send()

    @pl.when(is_boundary)
    def _():
        for v in range(2):
            for c in range(PIECES):
                for i in range(1, near):
                    far_out[v, c, i].wait_send()
                final[v, c].wait_send()


def fused(ep_count, tp_count, tokens, norm_gain, route_ids, route_weights, w_gate, w_up, w_down):
    rows, width = tokens.shape
    hidden = w_gate.shape[2]
    experts = ep_count * tp_count
    near = 2 * tp_count
    cap = 3 * rows * route_ids.shape[1] // (2 * experts)
    part_w = width // PIECES
    vmem = pl.BlockSpec(memory_space=pltpu.VMEM)
    hbm = pl.BlockSpec(memory_space=pl.ANY)

    def b16(*shape):
        return pltpu.VMEM(shape, jnp.bfloat16)

    def sems(*shape):
        return pltpu.SemaphoreType.DMA(shape)

    return pl.pallas_call(
        functools.partial(kernel, ep_count, tp_count, cap),
        out_shape=jax.ShapeDtypeStruct((rows, width), tokens.dtype),
        in_specs=[vmem] * 4 + [hbm] * 3,
        out_specs=vmem,
        scratch_shapes=[
            b16(PIECES, rows, part_w), pltpu.VMEM((2 * near, rows), jnp.float32),
            b16(near * cap, rows), b16(near * cap, rows),
            *[b16(near, cap, width)] * 4,
            b16(2, PIECES, rows, part_w), pltpu.VMEM((2, 2 * near, rows), jnp.float32),
            *[b16(2, near * cap, rows)] * 3,
            b16(2, PIECES, near, cap, part_w),
            b16(2, PIECES, tp_count, cap, part_w),
            b16(2, PIECES, tp_count, cap, part_w),
            b16(2, PIECES, near, cap, part_w),
            b16(2, PIECES, rows, part_w), b16(PIECES, rows, part_w),
            b16(width, hidden), b16(width, hidden), b16(hidden, width),
            pltpu.VMEM((rows, width), jnp.float32),
            sems(3), sems(PIECES), sems(2, PIECES), sems(1), sems(2),
            sems(near), sems(near), sems(near), sems(near),
            sems(2, PIECES, near), sems(2, PIECES, tp_count),
            sems(2, PIECES, tp_count), sems(2, PIECES, near),
            sems(2, PIECES), sems(PIECES),
        ],
        compiler_params=pltpu.CompilerParams(
            collective_id=0, has_side_effects=True, vmem_limit_bytes=56 * 1024 * 1024
        ),
    )(tokens, norm_gain.reshape(1, width), route_ids, route_weights, w_gate, w_up, w_down)


def solution(mesh):
    ep_count, tp_count = mesh.shape["ep"], mesh.shape["tp"]

    def on_device(*args):
        rows, experts = args[0].shape[0], ep_count * tp_count
        cap = 3 * rows * args[2].shape[1] // (2 * experts)
        if ep_count != 4 or tp_count != 4 or cap % 8 or rows % 128 or args[0].shape[1] % 256:
            return plain(*args)
        return fused(ep_count, tp_count, *args)

    return jax.shard_map(
        on_device,
        mesh=mesh,
        in_specs=(
            P(("grp", "ep", "tp"), None),
            P(),
            P(("grp", "ep", "tp"), None),
            P(("grp", "ep", "tp"), None),
            P(("ep", "tp"), None, None),
            P(("ep", "tp"), None, None),
            P(("ep", "tp"), None, None),
        ),
        out_specs=P(("grp", "ep", "tp"), None),
        check_vma=False,
    )
```

```python
import functools

import jax
import jax.numpy as jnp
from jax import lax
from jax.experimental import pallas as pl
from jax.experimental.pallas import tpu as pltpu
from jax.sharding import PartitionSpec as P

MESH = pl.DeviceIdType.MESH


def plain(tokens, norm_gain, route_ids, route_weights, w_gate, w_up, w_down):
    tok_rows, model_width = tokens.shape
    top_count = route_ids.shape[1]
    ep_count = lax.axis_size("ep")
    tp_count = lax.axis_size("tp")
    experts = ep_count * tp_count
    capacity = 3 * tok_rows * top_count // (2 * experts)
    values = tokens.astype(jnp.float32)
    normed = (
        values * lax.rsqrt(jnp.mean(values * values, axis=-1, keepdims=True) + 1e-06) * norm_gain
    ).astype(jnp.bfloat16)
    flat_ids = route_ids.reshape(-1)
    onehot = (flat_ids[:, None] == jnp.arange(experts, dtype=jnp.int32)[None, :]).astype(jnp.int32)
    slot_index = jnp.sum((jnp.cumsum(onehot, axis=0) - onehot) * onehot, axis=-1)
    token_of = jnp.arange(tok_rows * top_count, dtype=jnp.int32) // top_count
    buffer = jnp.zeros((experts, capacity, model_width), jnp.bfloat16)
    buffer = buffer.at[flat_ids, slot_index].set(normed[token_of])
    received = lax.all_to_all(buffer, ("ep", "tp"), split_axis=0, concat_axis=0, tiled=True)
    flat_rows = received.reshape(-1, model_width)
    gate_act = jnp.dot(flat_rows, w_gate[0], preferred_element_type=jnp.float32)
    up_act = jnp.dot(flat_rows, w_up[0], preferred_element_type=jnp.float32)
    hidden = (jax.nn.silu(gate_act) * up_act).astype(jnp.bfloat16)
    result = jnp.dot(hidden, w_down[0], preferred_element_type=jnp.float32).astype(jnp.bfloat16)
    returned = lax.all_to_all(
        result.reshape(received.shape), ("ep", "tp"), split_axis=0, concat_axis=0, tiled=True
    )
    picked = (
        returned[flat_ids, slot_index].reshape(tok_rows, top_count, model_width).astype(jnp.float32)
    )
    return jnp.sum(picked * route_weights[:, :, None], axis=1).astype(jnp.bfloat16)


def flipped(index, bits):
    bit = 1
    while bit <= bits:
        if bits & bit:
            index = index + (1 - 2 * ((index // bit) % 2)) * bit
        bit *= 2
    return index


PIECES = 4


def kernel(
    ep_count, tp_count, cap,
    x_hbm, gain_ref, ids_ref, wts_ref, wg_hbm, wu_hbm, wd_hbm, out_hbm,
    x_ref, out_ref, io_sem,
    normed, meta, share_hi, share_lo, nsend, nrecv, nres, nback,
    rblock, rmeta, rpick, rshare_hi, rshare_lo, fsend, frecv, fres, rback, rsend, farback,
    wg, wu, wd, acc,
    w_sem, dense_s, dense_r, meta_s, meta_r, near_s, near_r, nret_s, nret_r,
    far_s, far_r, fret_s, fret_r, final_s, final_r,
):
    ep, tp, grp = lax.axis_index("ep"), lax.axis_index("tp"), lax.axis_index("grp")
    rows, width = x_ref.shape
    part_w = width // PIECES
    top = ids_ref.shape[0]
    experts = ep_count * tp_count
    near = 2 * tp_count
    me = ep * tp_count + tp
    boundary = (ep + ep // 2) % 2
    wave_of_me = 1 - boundary
    own_relay, other_relay = 1 + ep // 2, 2 - ep // 2
    is_boundary, is_end = boundary == 1, boundary == 0

    def at(plane, j):
        return (grp, plane, flipped(tp, j))

    def remote(src, dst, s_sem, r_sem, target):
        return pltpu.make_async_remote_copy(
            src_ref=src, dst_ref=dst, send_sem=s_sem, recv_sem=r_sem,
            device_id=target, device_id_type=MESH,
        )

    barrier = pltpu.get_barrier_semaphore()

    def greet(target):
        pl.semaphore_signal(barrier, inc=1, device_id=target, device_id_type=MESH)

    greet(at(flipped(ep, 2), 0))

    @pl.when(is_boundary)
    def _():
        greet(at(flipped(ep, 3), 0))

    for g in range(near - 1, 0, -1):
        greet(at(flipped(ep, g // tp_count), g % tp_count))
    fetch = pltpu.make_async_copy(x_hbm, x_ref, io_sem.at[0])
    fetch.start()
    loads = [
        pltpu.make_async_copy(src.at[0], dst, w_sem.at[i])
        for i, (src, dst) in enumerate(((wg_hbm, wg), (wu_hbm, wu), (wd_hbm, wd)))
    ]
    for load in loads:
        load.start()

    planes = [ep, flipped(ep, 1)]
    dense = [
        remote(normed.at[c], rblock.at[wave_of_me, c], dense_s.at[c], dense_r.at[wave_of_me, c],
               at(other_relay, 0))
        for c in range(PIECES)
    ]
    meta_copy = remote(meta, rmeta.at[wave_of_me], meta_s.at[0], meta_r.at[wave_of_me],
                       at(other_relay, 0))
    stores = [
        pltpu.make_async_copy(
            out_ref.at[:, pl.ds(c * part_w, part_w)], out_hbm.at[:, pl.ds(c * part_w, part_w)],
            io_sem.at[1 + c])
        for c in range(PIECES)
    ]
    near_out = [
        remote(nsend.at[g], nrecv.at[g], near_s.at[g], near_r.at[g],
               at(planes[g // tp_count], g % tp_count))
        for g in range(near)
    ]
    near_ret = [
        remote(nres.at[g], nback.at[g], nret_s.at[g], nret_r.at[g],
               at(planes[g // tp_count], g % tp_count))
        for g in range(near)
    ]
    far_out, far_ret, final = {}, {}, {}
    for v in range(2):
        for c in range(PIECES):
            for i in range(near):
                far_out[v, c, i] = remote(
                    fsend.at[v, c, i], frecv.at[v, c, i % tp_count], far_s.at[v, c, i],
                    far_r.at[v, c, i % tp_count], at(planes[i // tp_count], i % tp_count))
            for j in range(tp_count):
                place = wave_of_me * tp_count + j
                far_ret[v, c, j] = remote(
                    fres.at[v, c, j], rback.at[v, c, place], fret_s.at[v, c, j],
                    fret_r.at[v, c, place], at(own_relay, j))
            final[v, c] = remote(rsend.at[v, c], farback.at[c], final_s.at[v, c], final_r.at[c],
                                 at(flipped(ep, 3 - v), 0))

    down = lax.broadcasted_iota(jnp.int32, (rows, rows), 0)
    across = lax.broadcasted_iota(jnp.int32, (rows, rows), 1)

    expert_of = lax.broadcasted_iota(jnp.int32, (experts, rows), 0) ^ me
    ids, wts = ids_ref[...], wts_ref[...]
    named = jnp.zeros((experts, rows), jnp.float32)
    weight = jnp.zeros((experts, rows), jnp.float32)
    for k in range(top):
        match = ids[k:k + 1] == expert_of
        named = named + jnp.where(match, 1.0, 0.0)
        weight = weight + jnp.where(match, wts[k:k + 1], 0.0)
    earlier = jnp.where(down < across, 1.0, 0.0).astype(jnp.bfloat16)
    rank = jnp.dot(named.astype(jnp.bfloat16), earlier, preferred_element_type=jnp.float32)
    rank = jnp.where(named > 0.5, rank, -1.0)
    meta[0:near] = rank[near:]
    meta[near:] = weight[near:]

    fetch.wait()
    values = x_ref[...].astype(jnp.float32)
    rows_normed = (
        values
        * lax.rsqrt(jnp.mean(values * values, axis=-1, keepdims=True) + 1e-06)
        * gain_ref[...]
    ).astype(jnp.bfloat16)
    for c in range(PIECES):
        normed[c] = rows_normed[:, c * part_w:(c + 1) * part_w]

    def onehots(rank, weight):
        slot = lax.broadcasted_iota(jnp.int32, (near, cap, rows), 1).astype(jnp.float32)
        taken = rank[:, None, :] == slot
        pick = jnp.where(taken, 1.0, 0.0).reshape(near * cap, rows).astype(jnp.bfloat16)
        share = jnp.where(taken, weight[:, None, :], 0.0).reshape(near * cap, rows)
        high = share.astype(jnp.bfloat16)
        return pick, high, (share - high.astype(jnp.float32)).astype(jnp.bfloat16)

    pl.semaphore_wait(barrier, near + boundary)

    @pl.when(is_boundary)
    def _():
        meta_copy.start()
        for c in range(PIECES):
            dense[c].start()

    pick, high, low = onehots(rank[:near], weight[:near])
    share_hi[...] = high
    share_lo[...] = low

    def pack_near(p):
        packed = jnp.dot(
            pick[p * tp_count * cap:(p + 1) * tp_count * cap], rows_normed,
            preferred_element_type=jnp.float32,
        ).astype(jnp.bfloat16).reshape(tp_count, cap, width)
        for j in range(tp_count):
            g = p * tp_count + j
            if g:
                nsend[g] = packed[j]
            else:
                nrecv[0] = packed[0]
        for j in range(tp_count):
            if p or j:
                near_out[p * tp_count + j].start()

    pack_near(1)

    @pl.when(is_end)
    def _():
        meta_copy.start()
        for c in range(PIECES):
            dense[c].start()

    pack_near(0)

    def hidden_of(gate_act, up_act):
        return (gate_act / (1.0 + jnp.exp(-gate_act)) * up_act).astype(jnp.bfloat16)

    def dot(a, b):
        return jnp.dot(a, b, preferred_element_type=jnp.float32)

    def expert_near(p):
        base = p * tp_count
        for g in range(base, base + tp_count):
            if g:
                near_out[g].wait_recv()
        block = nrecv[base:base + tp_count].reshape(tp_count * cap, width)
        hidden = hidden_of(dot(block, wg[...]), dot(block, wu[...]))
        result = dot(hidden, wd[...]).astype(jnp.bfloat16).reshape(tp_count, cap, width)
        for j in range(tp_count):
            if p or j:
                nres[base + j] = result[j]
            else:
                nback[0] = result[0]
        if p == 0:
            for j in range(1, tp_count):
                near_ret[j].start()

    def relay_out(v, c):
        @pl.when(is_boundary)
        def _():
            if c == 0:
                remote(meta, rmeta.at[v], meta_s.at[0], meta_r.at[v], at(other_relay, 0)).wait_recv()
                ranks, weights = rmeta[v, 0:near], rmeta[v, near:]
                if v == 0:
                    ranks = jnp.concatenate([ranks[tp_count:], ranks[:tp_count]], axis=0)
                    weights = jnp.concatenate([weights[tp_count:], weights[:tp_count]], axis=0)
                rp, rh, rl = onehots(ranks, weights)
                rpick[v] = rp
                rshare_hi[v] = rh
                rshare_lo[v] = rl
            remote(normed.at[c], rblock.at[v, c], dense_s.at[c], dense_r.at[v, c],
                   at(other_relay, 0)).wait_recv()
            packed = dot(rpick[v], rblock[v, c]).astype(jnp.bfloat16).reshape(near, cap, part_w)
            frecv[v, c, 0] = packed[0]
            for i in range(1, near):
                fsend[v, c, i] = packed[i]
            for i in list(range(tp_count, near)) + list(range(1, tp_count)):
                far_out[v, c, i].start()

    def expert_far(v):
        gate_act = up_act = None
        for c in range(PIECES):
            for j in range(1, tp_count):
                far_out[v, c, j].wait_recv()

            @pl.when(is_end)
            def _():
                far_out[v, c, tp_count].wait_recv()

            block = frecv[v, c].reshape(tp_count * cap, part_w)
            more_gate = dot(block, wg[c * part_w:(c + 1) * part_w])
            more_up = dot(block, wu[c * part_w:(c + 1) * part_w])
            gate_act = more_gate if c == 0 else gate_act + more_gate
            up_act = more_up if c == 0 else up_act + more_up
        hidden = hidden_of(gate_act, up_act)
        for c in range(PIECES):
            result = dot(hidden, wd[:, c * part_w:(c + 1) * part_w])
            result = result.astype(jnp.bfloat16).reshape(tp_count, cap, part_w)
            fres[v, c] = result
            for j in range(1, tp_count):
                far_ret[v, c, j].start()

            @pl.when(is_end)
            def _():
                far_ret[v, c, 0].start()

            @pl.when(is_boundary)
            def _():
                rback[v, c, 0] = fres[v, c, 0]

    def combine(high, low, block):
        total = None
        for comb in (high, low):
            term = lax.dot_general(
                comb, block, (((0,), (0,)), ((), ())), preferred_element_type=jnp.float32
            )
            total = term if total is None else total + term
        return total

    def relay_back(v, c):
        @pl.when(is_boundary)
        def _():
            for i in range(1, near):
                remote(fres.at[v, c, 0], rback.at[v, c, i], fret_s.at[v, c, 0],
                       fret_r.at[v, c, i], at(own_relay, 1)).wait_recv()
            block = rback[v, c].reshape(near * cap, part_w)
            rsend[v, c] = combine(rshare_hi[v], rshare_lo[v], block).astype(jnp.bfloat16)
            final[v, c].start()

    for load in loads:
        load.wait()
    def return_near(cond, js):
        @pl.when(cond)
        def _():
            for j in js:
                near_ret[tp_count + j].start()

    def return_near(cond, js):
        @pl.when(cond)
        def _():
            for j in js:
                near_ret[tp_count + j].start()

    expert_near(0)
    relay_out(0, 0)
    expert_near(1)
    return_near(is_end, range(tp_count))
    for c in range(1, PIECES):
        relay_out(0, c)
    expert_far(0)
    for c in range(PIECES):
        relay_out(1, c)
    return_near(is_boundary, range(tp_count))
    for c in range(PIECES):
        relay_back(0, c)
    expert_far(1)
    pass

    for g in range(1, near):
        near_ret[g].wait_recv()
    acc[...] = combine(share_hi[...], share_lo[...], nback[...].reshape(near * cap, width))
    for c in range(PIECES):
        relay_back(1, c)
    for c in range(PIECES):
        final[0, c].wait_recv()
        part = acc[:, c * part_w:(c + 1) * part_w] + farback[c].astype(jnp.float32)
        out_ref[:, c * part_w:(c + 1) * part_w] = part.astype(out_ref.dtype)
        stores[c].start()

    for store in stores:
        store.wait()
    meta_copy.wait_send()
    for copy in dense + near_out[1:] + near_ret[1:]:
        copy.wait_send()
    for v in range(2):
        for c in range(PIECES):
            for j in range(1, tp_count):
                far_ret[v, c, j].wait_send()

    @pl.when(is_end)
    def _():
        for v in range(2):
            for c in range(PIECES):
                far_ret[v, c, 0].wait_send()

    @pl.when(is_boundary)
    def _():
        for v in range(2):
            for c in range(PIECES):
                for i in range(1, near):
                    far_out[v, c, i].wait_send()
                final[v, c].wait_send()


def fused(ep_count, tp_count, tokens, norm_gain, route_ids, route_weights, w_gate, w_up, w_down):
    rows, width = tokens.shape
    hidden = w_gate.shape[2]
    experts = ep_count * tp_count
    near = 2 * tp_count
    cap = 3 * rows * route_ids.shape[1] // (2 * experts)
    part_w = width // PIECES
    vmem = pl.BlockSpec(memory_space=pltpu.VMEM)
    hbm = pl.BlockSpec(memory_space=pl.ANY)

    def b16(*shape):
        return pltpu.VMEM(shape, jnp.bfloat16)

    def sems(*shape):
        return pltpu.SemaphoreType.DMA(shape)

    return pl.pallas_call(
        functools.partial(kernel, ep_count, tp_count, cap),
        out_shape=jax.ShapeDtypeStruct((rows, width), tokens.dtype),
        in_specs=[hbm] + [vmem] * 3 + [hbm] * 3,
        out_specs=hbm,
        scratch_shapes=[
            b16(rows, width), b16(rows, width), sems(1 + PIECES),
            b16(PIECES, rows, part_w), pltpu.VMEM((2 * near, rows), jnp.float32),
            b16(near * cap, rows), b16(near * cap, rows),
            *[b16(near, cap, width)] * 4,
            b16(2, PIECES, rows, part_w), pltpu.VMEM((2, 2 * near, rows), jnp.float32),
            *[b16(2, near * cap, rows)] * 3,
            b16(2, PIECES, near, cap, part_w),
            b16(2, PIECES, tp_count, cap, part_w),
            b16(2, PIECES, tp_count, cap, part_w),
            b16(2, PIECES, near, cap, part_w),
            b16(2, PIECES, rows, part_w), b16(PIECES, rows, part_w),
            b16(width, hidden), b16(width, hidden), b16(hidden, width),
            pltpu.VMEM((rows, width), jnp.float32),
            sems(3), sems(PIECES), sems(2, PIECES), sems(1), sems(2),
            sems(near), sems(near), sems(near), sems(near),
            sems(2, PIECES, near), sems(2, PIECES, tp_count),
            sems(2, PIECES, tp_count), sems(2, PIECES, near),
            sems(2, PIECES), sems(PIECES),
        ],
        compiler_params=pltpu.CompilerParams(
            collective_id=0, has_side_effects=True, vmem_limit_bytes=56 * 1024 * 1024
        ),
    )(tokens, norm_gain.reshape(1, width), route_ids.T, route_weights.T, w_gate, w_up, w_down)


def solution(mesh):
    ep_count, tp_count = mesh.shape["ep"], mesh.shape["tp"]

    def on_device(*args):
        rows, experts = args[0].shape[0], ep_count * tp_count
        cap = 3 * rows * args[2].shape[1] // (2 * experts)
        if ep_count != 4 or tp_count != 4 or cap % 8 or rows % 128 or args[0].shape[1] % 256:
            return plain(*args)
        return fused(ep_count, tp_count, *args)

    return jax.shard_map(
        on_device,
        mesh=mesh,
        in_specs=(
            P(("grp", "ep", "tp"), None),
            P(),
            P(("grp", "ep", "tp"), None),
            P(("grp", "ep", "tp"), None),
            P(("ep", "tp"), None, None),
            P(("ep", "tp"), None, None),
            P(("ep", "tp"), None, None),
        ),
        out_specs=P(("grp", "ep", "tp"), None),
        check_vma=False,
    )
```
